32 devices in a mesh: sp: 4 (over y, x), tp: 8 (over z, core).
Axes of the slice: x: 2, y: 2, z: 4, core: 2. Of those that a mesh axis runs over, the one named last changes fastest.
Arguments:
- out_gate: bfloat16 [2048, 2048], P('sp', 'tp'), may hold values from -6 to 6
- in_gate: bfloat16 [2048, 2048], P('sp', 'tp'), may hold values from -6 to 6
- conv_input: bfloat16 [2048, 2048], P('sp', 'tp'), may hold values from -6 to 6
- conv_taps: bfloat16 [3, 2048], P(None, 'tp'), may hold values from -3.5 to 3.5
- documents: int32 [2048], P('sp'), may hold values from 0 to 2, never falling along the last dimension, each value on 1 to 1536 neighbouring positions
- out_weight: bfloat16 [2048, 2048], P('tp'), may hold values from -0.125 to 0.125
- residual: bfloat16 [2048, 2048], P(('sp', 'tp')), may hold values from -6 to 6
- norm_gain: bfloat16 [2048], replicated, may hold values from 0.099609375 to 1.8984375
- expert_ids: int32 [2048, 2], P(('sp', 'tp')), may hold values from 0 to 3, all different within a row; in each aligned block of 64 rows (0 to 63, 64 to 127, ...) at most 48 rows name the same one
- route_weights: float32 [2048, 2], P(('sp', 'tp')), may hold values from 0.1 to 1
- gate_weight: bfloat16 [4, 2048, 4096], P('sp', None, 'tp'), may hold values from -0.125 to 0.125
- up_weight: bfloat16 [4, 2048, 4096], P('sp', None, 'tp'), may hold values from -0.125 to 0.125
- down_weight: bfloat16 [4, 4096, 2048], P('sp', 'tp'), may hold values from -0.09375 to 0.09375
Outputs:
- layer_out: bfloat16 [2048, 2048], P(('sp', 'tp'))
The draws below stay inside these ranges and needn't reach their ends.
Inputs may be any that keep to these rules, and one draw needn't show every extreme that they name: `expert_ids`: A token's two experts differ; in each aligned block of 64 rows no expert is named by more than 48 entries, a bound that some block reaches. `documents`: document numbers never fall along the sequence; a document holds at most 1536 positions.
All inputs are finite; a program needn't handle non-finite values.
Results may differ from the reference program's by a relative error of at most 0.017.
Values may be sent and summed in bfloat16 or wider, within the bound.
A program may use at most 64 MiB of HBM per device.

```python
import math
import jax
import jax.numpy as jnp
import numpy as np
from jax import lax

D = 2048
F = 4096
TAPS = 3
TOK_DEV = 512
TOKENS = 2048
EXPERTS = 4
ROWS = 64
CAP = 48
N_SP = 4
N_TP = 8


def steps_of(own_key, extent, split, low, top_value):
    level = 1.0
    for axis_at, blocks in split:
        draws = jax.random.uniform(jax.random.fold_in(jax.random.fold_in(own_key, 6), axis_at), (blocks,), jnp.float32, low / len(split), top_value / len(split))
        level = level * jnp.repeat(jnp.exp(draws), extent[axis_at] // blocks).reshape((-1,) + (1,) * (len(extent) - 1 - axis_at))
    return level


def profile(number_of, total, bound, skew):
    loads = [(1 << 20) // math.isqrt(rank ** skew) + 1 for rank in range(2, number_of + 1)]
    rest, counts = total - bound - (number_of - 1), [1] * (number_of - 1)
    while rest > 0:
        free = [i for i in range(number_of - 1) if counts[i] < bound]
        pool, left = sum([loads[i] for i in free]), rest
        for i in free:
            extra = min(bound - counts[i], max(1, left * loads[i] // pool), rest)
            counts[i] = counts[i] + extra
            rest = rest - extra
    return np.array([bound] + counts)


def uneven(stream_key, number_of, total, most, lean):
    if number_of == 2:
        one = jax.random.randint(stream_key, (), max(1, total - most), min(most, total - 1) + 1)
        return jnp.stack([one, total - one])
    sizes = jnp.asarray(profile(number_of, total, most, lean), jnp.int32)
    couples = (number_of - 1) // 2
    source_of, taker = sizes[1:1 + 2 * couples:2], sizes[2:2 + 2 * couples:2]
    margin = jnp.minimum(source_of - 1, most - taker)
    shifted = jax.random.randint(jax.random.fold_in(stream_key, 1), (couples,), 0, 1 << 20) % (margin + 1)
    sizes = sizes.at[1:1 + 2 * couples:2].set(source_of - shifted).at[2:2 + 2 * couples:2].set(taker + shifted)
    return sizes[jax.random.permutation(jax.random.fold_in(stream_key, 2), number_of)]


def shared_out(key, own, number, rows, count, top, bound, lean):
    ranking = jax.random.permutation(key, count)
    packed, usual = shares(count, rows * top, bound, lean, True), shares(count, rows * top, bound, lean, False)
    places = jnp.arange(count)

    def named(tallies, rotation):
        used = int((tallies > 0).sum())
        fixed = max(1, used // 4)
        passed = fixed + (places - fixed + rotation * (used - fixed)) % max(1, count - fixed)
        return jnp.zeros((count,), jnp.int32).at[ranking[jnp.where(places < fixed, places, passed)]].set(jnp.asarray(tallies, jnp.int32))

    tallies = jnp.where(number % 4 == 0, named(packed, number // 4), named(usual, number - number // 4 - 1))
    mixed = jax.random.permutation(jax.random.fold_in(own, 3), count)
    source_of, taker = mixed[0:count // 2 * 2:2], mixed[1:count // 2 * 2:2]
    slack = jnp.minimum(tallies[source_of] - 1, bound - tallies[taker]) // 2
    slack = jnp.where((source_of == ranking[0]) | (taker == ranking[0]) | (tallies[taker] == 0), 0, jnp.maximum(slack, 0))
    passed = jax.random.randint(jax.random.fold_in(own, 4), (count // 2,), 0, 1 << 20) % (slack + 1)
    tallies = tallies.at[source_of].add(-passed).at[taker].add(passed)
    labels = jnp.searchsorted(jnp.cumsum(tallies), jnp.arange(rows * top), side="right").astype(jnp.int32)
    table = labels.reshape(top, rows).T
    table = table[jax.random.permutation(jax.random.fold_in(own, 1), rows)]
    rotation = jax.random.randint(jax.random.fold_in(own, 2), (rows, 1), 0, top)
    return jnp.take_along_axis(table, (jnp.arange(top)[None, :] + rotation) % top, axis=1)


def shares(number_of, total, limit, lean, full):
    weights = [(1 << 20) // math.isqrt(grade ** lean) + 1 for grade in range(1, number_of + 1)]
    largest = limit if full else min(limit, max(-(-total // number_of), total * weights[0] // sum(weights)))
    least = 1 if total - largest >= number_of - 1 else 0
    counts, spare = [largest] + [least] * (number_of - 1), total - largest - least * (number_of - 1)
    while spare > 0:
        free = [i for i in range(1, number_of) if counts[i] < largest] or [i for i in range(1, number_of) if counts[i] < limit]
        whole, budget = sum([weights[i] for i in free]), spare
        for i in free:
            addition = min(limit - counts[i], max(1, budget * weights[i] // whole), spare)
            counts[i] = counts[i] + addition
            spare = spare - addition
    return np.array(counts)


def noise(key, shape, deviation, most, pieces=(), kind=jnp.bfloat16):
    gain = steps_of(key, shape, pieces, -0.22, 0.18) if pieces else 1.0
    array = jax.random.normal(key, shape, jnp.float32) * deviation * gain
    return jnp.minimum(jnp.maximum(array, -most), most).astype(kind)


def setup_inputs(seed: int = 0) -> dict:
    streams_of = jax.random.split(jax.random.key(seed), 14)
    out_gate = noise(streams_of[0], (TOKENS, D), 1.0, 6.0, ((0, 4), (1, 8)))
    in_gate = noise(streams_of[1], (TOKENS, D), 1.0, 6.0, ((0, 4), (1, 8)))
    conv_input = noise(streams_of[2], (TOKENS, D), 1.0, 6.0, ((0, 4), (1, 8)))
    conv_taps = noise(streams_of[3], (TAPS, D), TAPS ** -0.5, 3.5, ((1, 8),))
    documents = jnp.searchsorted(jnp.cumsum(uneven(streams_of[4], N_SP // 2 + 1, TOKENS, 3 * TOK_DEV, 0)), jnp.arange(TOKENS), side="right").astype(jnp.int32)
    out_weight = noise(streams_of[5], (D, D), D ** -0.5, 0.125, ((0, 8),))
    residual = noise(streams_of[6], (TOKENS, D), 1.0, 6.0, ((0, 32),))
    norm_gain = jnp.clip(1.0 + 0.18 * jax.random.normal(streams_of[7], (D,), jnp.float32), 0.099609375, 1.8984375).astype(jnp.bfloat16)
    expert_ids_keys = jax.random.split(jax.random.fold_in(streams_of[8], 1), TOKENS // ROWS)
    expert_ids_turns = jax.random.permutation(jax.random.fold_in(streams_of[8], 3), TOKENS // ROWS)
    expert_ids = jax.vmap(lambda own, number: shared_out(jax.random.fold_in(streams_of[8], 2), own, number, ROWS, EXPERTS, 2, CAP, 2))(expert_ids_keys, expert_ids_turns).reshape((TOKENS, 2))
    route_weights = jnp.clip(0.1 + 0.9 * jax.random.uniform(streams_of[9], (TOKENS, 2), jnp.float32) ** steps_of(streams_of[9], (TOKENS, 2), ((0, 32),), -0.2, 0.2), 0.1, 1.0)
    gate_weight = noise(streams_of[10], (EXPERTS, D, F), D ** -0.5, 0.125, ((0, 4), (2, 8)))
    up_weight = noise(streams_of[11], (EXPERTS, D, F), D ** -0.5, 0.125, ((0, 4), (2, 8)))
    down_weight = noise(streams_of[12], (EXPERTS, F, D), F ** -0.5, 0.09375, ((0, 4), (1, 8)))
    return dict(out_gate=out_gate, in_gate=in_gate, conv_input=conv_input, conv_taps=conv_taps, documents=documents, out_weight=out_weight, residual=residual, norm_gain=norm_gain, expert_ids=expert_ids, route_weights=route_weights, gate_weight=gate_weight, up_weight=up_weight, down_weight=down_weight)


EPS = 1e-06

def slot_index(expert_ids, experts, capacity):
    listed = expert_ids.reshape(-1).astype(jnp.int32)
    onehot = (listed[:, None] == jnp.arange(experts, dtype=jnp.int32)[None, :]).astype(jnp.int32)
    earlier = (jnp.cumsum(onehot, axis=0) - onehot).astype(jnp.int32)
    within = lax.optimization_barrier(jnp.sum(earlier * onehot, axis=1)).astype(jnp.int32)
    return (listed * capacity + within).astype(jnp.int32)

def dispatch_block(target, block_rows):
    count = block_rows.shape[0]
    slots = jnp.arange(EXPERTS * CAP, dtype=jnp.int32)
    table = lax.optimization_barrier(jnp.sum((target.reshape(count, 2)[:, :, None] == slots[None, None, :]).astype(jnp.float32), axis=1))
    placed = lax.dot_general(table, block_rows.astype(jnp.float32), (((0,), (0,)), ((), ())))
    return placed.astype(jnp.bfloat16)

def run_expert(operands):
    expert_in, gate_part, up_part, down_part = operands
    gate_proj = jnp.dot(expert_in, gate_part, preferred_element_type=jnp.float32)
    up_proj = jnp.dot(expert_in, up_part, preferred_element_type=jnp.float32)
    act = (jax.nn.silu(gate_proj) * up_proj).astype(jnp.bfloat16)
    width = F // N_TP

    def add_block(total, index):
        columns = lax.dynamic_slice_in_dim(act, index * width, width, 1)
        weight_rows = lax.dynamic_slice_in_dim(down_part, index * width, width, 0)
        partial_sum = lax.optimization_barrier(jnp.dot(columns, weight_rows, preferred_element_type=jnp.float32).astype(jnp.bfloat16))
        return (total + partial_sum.astype(jnp.float32), None)
    total, ignored = lax.scan(add_block, jnp.zeros((expert_in.shape[0], D), jnp.float32), jnp.arange(N_TP, dtype=jnp.int32))
    return total.astype(jnp.bfloat16)

def reference(out_gate, in_gate, conv_input, conv_taps, documents, out_weight, residual, norm_gain, expert_ids, route_weights, gate_weight, up_weight, down_weight):
    length = conv_input.shape[0]
    signal = in_gate.astype(jnp.float32) * conv_input.astype(jnp.float32)
    tap_values = conv_taps.astype(jnp.float32)
    position = jnp.arange(length, dtype=jnp.int32)
    mixed_conv = tap_values[2][None, :] * signal
    for offset in (1, 2):
        earlier_signal = jnp.pad(signal, ((offset, 0), (0, 0)))[:length]
        earlier_docs = jnp.pad(documents, (offset, 0))[:length]
        allowed = (position >= offset) & (earlier_docs == documents)
        mixed_conv = mixed_conv + jnp.where(allowed[:, None], tap_values[2 - offset][None, :] * earlier_signal, 0.0)
    gated = (out_gate.astype(jnp.float32) * mixed_conv).astype(jnp.bfloat16)
    width = D // N_TP

    def add_block(total, index):
        columns = lax.dynamic_slice_in_dim(gated, index * width, width, 1)
        weight_rows = lax.dynamic_slice_in_dim(out_weight, index * width, width, 0)
        partial_sum = lax.optimization_barrier(jnp.dot(columns, weight_rows, preferred_element_type=jnp.float32).astype(jnp.bfloat16))
        return (total + partial_sum.astype(jnp.float32), None)
    mixed, ignored = lax.scan(add_block, jnp.zeros((length, D), jnp.float32), jnp.arange(N_TP, dtype=jnp.int32))
    hidden_state = (residual.astype(jnp.float32) + mixed).astype(jnp.bfloat16)
    hidden_wide = hidden_state.astype(jnp.float32)
    stats = lax.optimization_barrier(jnp.mean(hidden_wide * hidden_wide, axis=-1, keepdims=True))
    normed = (hidden_wide * lax.rsqrt(stats + EPS) * norm_gain.astype(jnp.float32)[None, :]).astype(jnp.bfloat16)
    block_count = N_SP * N_TP
    normed_blocks = normed.reshape(block_count, ROWS, D)
    route_blocks = expert_ids.reshape(block_count, ROWS, 2)
    targets = jax.vmap(lambda ids: slot_index(ids, EXPERTS, CAP))(route_blocks)
    buffers = jax.vmap(dispatch_block)(targets, normed_blocks)
    expert_rows = buffers.reshape(block_count, EXPERTS, CAP, D).transpose(1, 0, 2, 3).reshape(EXPERTS, block_count * CAP, D)
    expert_out = lax.map(run_expert, (expert_rows, gate_weight, up_weight, down_weight))
    returned = expert_out.reshape(EXPERTS, block_count, CAP, D).transpose(1, 0, 2, 3).reshape(block_count, EXPERTS * CAP, D)
    picked = jax.vmap(lambda table, target: table[target])(returned, targets)
    picked = picked.astype(jnp.float32).reshape(block_count, ROWS, 2, D)
    weights = route_weights.astype(jnp.float32).reshape(block_count, ROWS, 2)
    combined = lax.optimization_barrier(jnp.sum(picked * weights[:, :, :, None], axis=2)).reshape(length, D)
    return (hidden_wide + combined).astype(jnp.bfloat16)
```

```python
import functools

import jax
import jax.numpy as jnp
from jax import lax
from jax.experimental import pallas as pl
from jax.experimental.pallas import tpu as pltpu
from jax.sharding import PartitionSpec as P

EPS = 1e-06


MESH = pl.DeviceIdType.MESH
CHUNK = 16
COLS = 512
UNITS = 256
HALO = 8
PIECE = 32
LAG = 2
LANES = 128
VMEM_LIMIT = 63 * 1024 * 1024


def where_am_i():
    s, t = lax.axis_index("sp"), lax.axis_index("tp")
    return s, t // 2, t % 2


def greet(s, z, c, n_sp, nz):
    barrier = pltpu.get_barrier_semaphore()
    peers = [(s, 2 * z + 1 - c)]
    peers += [(s, 2 * lax.rem(z + i, nz) + c) for i in range(1, nz)]
    peers += [(lax.rem(s + k, n_sp), 2 * z + c) for k in range(1, n_sp)]
    for peer in peers:
        pl.semaphore_signal(barrier, inc=1, device_id=peer, device_id_type=MESH)
    return lambda: pl.semaphore_wait(barrier, len(peers))


def link(src, dst, send_sem, recv_sem, peer):
    return pltpu.make_async_remote_copy(
        src_ref=src,
        dst_ref=dst,
        send_sem=send_sem,
        recv_sem=recv_sem,
        device_id=peer,
        device_id_type=MESH,
    )


def by_rows(first, count, body):
    def step(r, carry):
        body(pl.ds(pl.multiple_of(first + r * CHUNK, CHUNK), CHUNK))
        return carry

    lax.fori_loop(0, count // CHUNK, step, 0)


def by_columns(width, body):
    def step(r, carry):
        body(pl.ds(pl.multiple_of(r * COLS, COLS), COLS))
        return carry

    lax.fori_loop(0, width // COLS, step, 0)


def slot_hits(meta, experts, cap):
    rows = meta.shape[1]
    slots = lax.broadcasted_iota(jnp.int32, (len(experts) * cap, rows), 0).astype(jnp.float32)
    hits = []
    for k in range(2):
        at = jnp.full((1, rows), -1.0, jnp.float32)
        for a, expert in enumerate(experts):
            at = jnp.where(meta[2 * k : 2 * k + 1, :] == expert, float(a * cap) + meta[2 * k + 1 : 2 * k + 2, :], at)
        hits.append(slots == at)
    return hits


def slot_table(meta, experts, cap):
    first, second = slot_hits(meta, experts, cap)
    return (first | second).astype(jnp.float32).astype(jnp.bfloat16)


def slot_weights(meta, experts, cap):
    first, second = slot_hits(meta, experts, cap)
    weights = jnp.where(first, meta[4:5, :], 0.0) + jnp.where(second, meta[5:6, :], 0.0)
    high = weights.astype(jnp.bfloat16)
    return high, (weights - high.astype(jnp.float32)).astype(jnp.bfloat16)


def weigh(weights, values):
    dims = (((0,), (0,)), ((), ()))
    total = lax.dot_general(weights[0], values, dims, preferred_element_type=jnp.float32)
    return total + lax.dot_general(weights[1], values, dims, preferred_element_type=jnp.float32)


def describe(ids, shares, meta, n_sp):
    rows = ids.shape[1]
    named_ids = ids[...].astype(jnp.float32)
    choice = [named_ids[0:1, :], named_ids[1:2, :]]
    expert = lax.broadcasted_iota(jnp.int32, (-(-n_sp // CHUNK) * CHUNK, rows), 0).astype(jnp.float32)
    names = [expert == choice[0], expert == choice[1]]
    named = (names[0] | names[1]).astype(jnp.float32).astype(jnp.bfloat16)
    before = lax.broadcasted_iota(jnp.int32, (rows, rows), 0) < lax.broadcasted_iota(jnp.int32, (rows, rows), 1)
    earlier = jnp.dot(
        named, before.astype(jnp.float32).astype(jnp.bfloat16), preferred_element_type=jnp.float32
    )
    for k in range(2):
        meta[2 * k : 2 * k + 1, :] = choice[k]
        meta[2 * k + 1 : 2 * k + 2, :] = jnp.sum(jnp.where(names[k], earlier, 0.0), axis=0, keepdims=True)
    meta[4:6, :] = shares[...]
    meta[6:8, :] = jnp.zeros((2, rows), jnp.float32)


def layer_kernel(
    n_sp, nz, cap,
    in_gate_hbm, conv_input_hbm, out_gate_hbm, taps_hbm, docs_hbm, out_weight_hbm, residual_hbm, gain_hbm, ids_hbm,
    shares_hbm, gate_hbm, up_hbm, down_hbm,
    out,
    in_gate, conv_input, out_gate, taps, docs, residual, gain, ids, shares, gate, up, down,
    signal, long_docs, tail_signal, tail_docs, halo_signal, halo_docs,
    gated, other_gated, weight, part, from_low, from_high, to_high, to_low, hidden, nbuf,
    meta, metas, side_metas, raw, routed, gathered, act, half_rx, arrived, side_sum, side_rx, mine, combined, zrx,
    w_sem, h_send, h_recv, m_send, m_recv, x_send, x_recv, v_send, v_recv, o_send, o_recv,
    u_send, u_recv, d_send, d_recv, g_send, g_recv, p_send, p_recv, f_send, f_recv,
    e_send, e_recv, r_send, r_recv, k_send, k_recv, b_send, b_recv,
):
    s, z, c = where_am_i()
    o = 1 - c
    relayed = n_sp == 4
    partner = (s, 2 * z + o)
    rows, width = residual.shape
    length, channels = in_gate.shape
    piece = min(PIECE, rows)
    per = rows // piece
    pieces = nz * per
    greeted = greet(s, z, c, n_sp, nz)
    loads = [
        pltpu.make_async_copy(src, dst, w_sem.at[i])
        for i, (src, dst) in enumerate(
            [
                (in_gate_hbm, in_gate), (conv_input_hbm, conv_input), (docs_hbm, docs), (taps_hbm, taps),
                (ids_hbm, ids), (shares_hbm, shares), (out_gate_hbm, out_gate), (out_weight_hbm, weight.at[0]),
                (residual_hbm, residual), (gain_hbm, gain), (gate_hbm, gate), (up_hbm, up), (down_hbm, down),
            ]
        )
    ]
    for load in loads:
        load.start()

    @pl.when(z == 0)
    def no_lower():
        from_low[...] = jnp.zeros_like(from_low)

    @pl.when(z == nz - 1)
    def no_higher():
        from_high[...] = jnp.zeros_like(from_high)

    def above(i):
        return lax.rem(z + i, nz)

    def on_plane(k):
        return lax.rem(s + k, n_sp)

    if relayed:
        right, down_one = 1 - 2 * (s % 2), 2 - 4 * (s // 2)
        side = s + (1 - c) * right + c * down_one
        cross = s + c * right + (1 - c) * down_one
        side_peer, cross_peer = (side, 2 * z + c), (cross, 2 * z + c)
        experts = [s.astype(jnp.float32), cross.astype(jnp.float32)]
    else:
        experts = [on_plane(k).astype(jnp.float32) for k in range(n_sp)]

    for load in loads[:6]:
        load.wait()
    signal[HALO:, :] = in_gate[...].astype(jnp.float32) * conv_input[...].astype(jnp.float32)
    row = jnp.broadcast_to(docs[...].astype(jnp.float32).reshape(1, length), (CHUNK, length))
    one = (lax.broadcasted_iota(jnp.int32, (CHUNK, LANES), 0) == 0).astype(jnp.float32).astype(jnp.bfloat16)
    long_docs[HALO:, :] = lax.dot_general(
        row.astype(jnp.bfloat16), one, (((0,), (0,)), ((), ())), preferred_element_type=jnp.float32
    )
    tail_signal[...] = signal[length : length + HALO, :]
    tail_docs[...] = long_docs[length : length + HALO, :]
    describe(ids, shares, meta, n_sp)
    metas[z] = meta[...]
    loads[6].wait()
    tap_values = taps[...].astype(jnp.float32)

    def convolve(strip):
        r = strip * rows
        at = [slice(HALO + r - j, HALO + r - j + rows) for j in range(3)]
        here = long_docs[at[0], :]
        same = [None] + [long_docs[at[j], :] == here for j in (1, 2)]
        for l in range(0, channels, LANES):
            lane = slice(l, l + LANES)
            conv = tap_values[2:3, lane] * signal[at[0], lane]
            for j in (1, 2):
                conv = conv + jnp.where(same[j], tap_values[2 - j : 3 - j, lane] * signal[at[j], lane], 0.0)
            gated[strip, :, lane] = (out_gate[r : r + rows, lane].astype(jnp.float32) * conv).astype(jnp.bfloat16)

    for strip in range(2 * nz - 1, 0, -1):
        convolve(strip)
    loads[7].wait()
    greeted()
    following = (on_plane(1), 2 * z + c)
    halo = [
        link(tail_signal, halo_signal, h_send.at[0], h_recv.at[0], following),
        link(tail_docs, halo_docs, h_send.at[1], h_recv.at[1], following),
    ]
    given = [
        link(gated.at[2 * b + o], other_gated.at[b], o_send.at[b], o_recv.at[b], partner) for b in range(nz)
    ]
    lent = link(weight.at[0], weight.at[1], v_send.at[0], v_recv.at[0], partner)
    given[nz - 1].start()
    lent.start()
    for copy in halo:
        copy.start()
    for b in range(nz - 2, 0, -1):
        given[b].start()

    def note(i):
        return link(meta, metas.at[z], m_send.at[i], m_recv.at[z], (s, 2 * above(i) + c))

    def noted(i):
        return link(meta, metas.at[above(i)], m_send.at[i], m_recv.at[above(i)], (s, 2 * above(i) + c))

    for i in range(1, nz):
        note(i).start()
    side_note = link(metas, side_metas, x_send.at[0], x_recv.at[0], side_peer) if relayed else None

    def place(q):
        return nz - 1 - q // per, (q % per) * piece

    def upward(q):
        b, first = place(q)
        at = pl.ds(first, piece)
        return link(to_high.at[b, at], from_low.at[b, at], u_send.at[q], u_recv.at[q], (s, 2 * above(1) + c))

    def downward(q):
        b, first = place(q)
        at = pl.ds(first, piece)
        return link(to_low.at[b, at], from_high.at[b, at], d_send.at[q], d_recv.at[q], (s, 2 * above(nz - 1) + c))

    def pass_on(q, came, going, copy):
        b, first = place(q)

        def add(r):
            going[b, r, :] = (part[b, r, :] + came[b, r, :].astype(jnp.float32)).astype(jnp.bfloat16)

        by_rows(first, piece, add)
        copy(q).start()

    def project(b):
        given[b].wait_recv()

        def columns(cols):
            part[b, :, cols] = jnp.dot(
                gated[2 * b + c], weight[0, :, cols], preferred_element_type=jnp.float32
            ) + jnp.dot(other_gated[b], weight[1, :, cols], preferred_element_type=jnp.float32)

        by_columns(width, columns)

        @pl.when(z == b)
        def own():
            def add(r):
                part[b, r, :] = part[b, r, :] + residual[r, :].astype(jnp.float32)

            by_rows(0, rows, add)

    lent.wait_recv()
    loads[8].wait()
    for b in range(nz - 1, -1, -1):
        if b == 0:
            for copy in halo:
                copy.wait_recv()
            signal[:HALO, :] = halo_signal[...]
            long_docs[:HALO, :] = jnp.where(s == 0, -1.0, halo_docs[...])
            convolve(0)
            given[0].start()
        project(b)
        for q in range((nz - 1 - b) * per, (nz - b) * per):

            @pl.when(z == 0)
            def lowest(q=q):
                pass_on(q, from_low, to_high, upward)

            @pl.when(z == nz - 1)
            def highest(q=q):
                pass_on(q, from_high, to_low, downward)

    for i in range(1, nz):
        noted(i).wait_recv()
    if relayed:
        side_note.start()
    loads[9].wait()

    def from_below(q):
        @pl.when(z > 0)
        def some():
            upward(q).wait_recv()

        @pl.when((z > 0) & (z < nz - 1))
        def middle():
            pass_on(q, from_low, to_high, upward)

    def from_above(q):
        @pl.when(z < nz - 1)
        def some():
            downward(q).wait_recv()

        @pl.when((z > 0) & (z < nz - 1))
        def middle():
            pass_on(q, from_high, to_low, downward)

    def norm(q):
        b, first = place(q)

        def rows_of(r):
            total = part[b, r, :] + from_low[b, r, :].astype(jnp.float32) + from_high[b, r, :].astype(jnp.float32)
            state = total.astype(jnp.bfloat16)
            hidden[b, r, :] = state
            wide = state.astype(jnp.float32)
            stats = jnp.mean(wide * wide, axis=-1, keepdims=True)
            scale = gain[...].astype(jnp.float32).reshape(1, width)
            nbuf[b, r, :] = (wide * lax.rsqrt(stats + EPS) * scale).astype(jnp.bfloat16)

        by_rows(first, piece, rows_of)

    def raw_copy(b):
        return link(nbuf.at[b], raw.at[b], g_send.at[b], g_recv.at[b], side_peer)

    def slot_copies(b, those=(0, 1)):
        if relayed:
            return [
                link(routed.at[b, k], gathered.at[b, 0, 2 + k], p_send.at[b, k], p_recv.at[b, k], cross_peer)
                for k in those
            ]
        return [
            link(
                routed.at[b, k], gathered.at[b, 0, k], p_send.at[b, k], p_recv.at[b, k], (on_plane(k), 2 * z + c)
            )
            for k in range(1, n_sp)
        ]

    def dispatch(b):
        if relayed:
            raw_copy(b).start()
        table = slot_table(metas[b], experts, cap)

        def columns(cols):
            placed = jnp.dot(table, nbuf[b, :, cols], preferred_element_type=jnp.float32).astype(jnp.bfloat16)
            gathered[b, 0, 0, :, cols] = placed[:cap]
            for k in range(1, len(experts)):
                routed[b, k - 1 if relayed else k, :, cols] = placed[k * cap : (k + 1) * cap]

        by_columns(width, columns)
        for copy in slot_copies(b, (0,)):
            copy.start()

    def relay(b):
        if not relayed:
            return
        raw_copy(b).wait_recv()
        table = slot_table(side_metas[b], experts, cap)

        def columns(cols):
            placed = jnp.dot(table, raw[b, :, cols], preferred_element_type=jnp.float32).astype(jnp.bfloat16)
            gathered[b, 0, 1, :, cols] = placed[:cap]
            routed[b, 1, :, cols] = placed[cap:]

        by_columns(width, columns)
        slot_copies(b, (1,))[0].start()

    def unless_own(b, act_on):
        @pl.when(z != b)
        def other():
            act_on(b)

    for t in range(pieces + LAG):

        @pl.when(z < nz // 2)
        def lower(t=t):
            if t < pieces:
                from_below(t)
            if t >= LAG:
                from_above(t - LAG)

        @pl.when(z >= nz // 2)
        def upper(t=t):
            if t < pieces:
                from_above(t)
            if t >= LAG:
                from_below(t - LAG)

        q = t - LAG
        if q >= 0:
            if q == 0 and relayed:
                side_note.wait_recv()
            norm(q)
            if q % per == per - 1:
                b = place(q)[0]
                unless_own(b, dispatch)
                if b < nz - 1:
                    unless_own(b + 1, relay)
    dispatch(z)
    unless_own(0, relay)
    relay(z)

    def at_step(j):
        if j == nz - 1:
            return z
        return nz - 1 - j - jnp.where(j >= nz - 1 - z, 1, 0)

    def forward(b):
        return link(gathered.at[b, 0], gathered.at[b, 1], f_send.at[b], f_recv.at[b], partner)

    def swap(b):
        return link(gathered.at[b, 0], half_rx.at[b], e_send.at[b], e_recv.at[b], partner)

    def return_copies(b):
        if relayed:
            return [
                link(routed.at[b, pl.ds(2, 2)], arrived.at[b], r_send.at[b, 0], r_recv.at[b, 0], cross_peer)
            ]
        return [
            link(
                routed.at[b, k], arrived.at[b, k], r_send.at[b, k], r_recv.at[b, k], (on_plane(n_sp - k), 2 * z + c)
            )
            for k in range(1, n_sp)
        ]

    def side_copy(b):
        return link(side_sum.at[b], side_rx.at[b], k_send.at[b], k_recv.at[b], side_peer)

    def gather(j):
        b = at_step(j)
        for copy in slot_copies(b):
            copy.wait_recv()
        forward(b).start()

    def expert(j):
        b = at_step(j)
        if j == 0:
            for load in loads[10:]:
                load.wait()
        forward(b).wait_recv()
        half = n_sp * cap
        hidden_units = gate.shape[1]
        step = min(UNITS, hidden_units)

        def inner(r, carry):
            units = pl.ds(pl.multiple_of(r * step, step), step)
            held = gathered[b].reshape(2 * half, width)
            gate_proj = jnp.dot(held, gate[:, units], preferred_element_type=jnp.float32)
            up_proj = jnp.dot(held, up[:, units], preferred_element_type=jnp.float32)
            act[:, units] = (gate_proj / (1.0 + jnp.exp(-gate_proj)) * up_proj).astype(jnp.bfloat16)
            return carry

        lax.fori_loop(0, hidden_units // step, inner, 0)
        for copy in slot_copies(b):
            copy.wait_send()
        forward(b).wait_send()

        def outer(cols):
            share = jnp.dot(act[...], down[:, cols], preferred_element_type=jnp.float32).astype(jnp.bfloat16)
            routed[b, :, :, cols] = share[:half].reshape(n_sp, cap, COLS)
            gathered[b, 0, :, :, cols] = share[half:].reshape(n_sp, cap, COLS)

        by_columns(width, outer)
        swap(b).start()

    def give_back(j):
        b = at_step(j)
        swap(b).wait_recv()

        def add(first, count):
            def columns(cols):
                at = pl.ds(first, count)
                total = routed[b, at, :, cols].astype(jnp.float32) + half_rx[b, at, :, cols].astype(jnp.float32)
                routed[b, at, :, cols] = total.astype(jnp.bfloat16)

            by_columns(width, columns)

        if relayed:
            add(2, 2)
        else:
            add(0, n_sp)
        for copy in return_copies(b):
            copy.start()
        if relayed:
            add(0, 2)

    def relay_back(j):
        if not relayed:
            return
        b = at_step(j)
        return_copies(b)[0].wait_recv()
        weights = slot_weights(side_metas[b], experts, cap)

        def columns(cols):
            values = jnp.concatenate([routed[b, 1, :, cols], arrived[b, 1, :, cols]], axis=0)
            side_sum[b, :, cols] = weigh(weights, values).astype(jnp.bfloat16)

        by_columns(width, columns)
        side_copy(b).start()

    def homeward(b):
        return link(combined.at[b], zrx.at[z], b_send.at[b], b_recv.at[z], (s, 2 * b + c))

    def collect(j):
        b = at_step(j)
        if relayed:
            side_copy(b).wait_recv()
        else:
            for copy in return_copies(b):
                copy.wait_recv()
        weights = slot_weights(metas[b], experts, cap)

        def columns(cols):
            parts = [routed[b, 0, :, cols]]
            if relayed:
                parts.append(arrived[b, 0, :, cols])
            else:
                parts += [arrived[b, k, :, cols] for k in range(1, n_sp)]
            total = weigh(weights, jnp.concatenate(parts, axis=0))
            if relayed:
                total = total + side_rx[b, :, cols].astype(jnp.float32)
            if j < nz - 1:
                combined[b, :, cols] = total.astype(jnp.bfloat16)
            else:
                mine[:, cols] = total

        by_columns(width, columns)
        if j < nz - 1:
            homeward(b).start()

    gather(0)
    for j in range(nz):
        if j + 1 < nz:
            gather(j + 1)
        expert(j)
        if j >= 1:
            relay_back(j - 1)
        give_back(j)
        if j >= 2:
            collect(j - 2)
    relay_back(nz - 1)
    if nz > 1:
        collect(nz - 2)
    collect(nz - 1)

    def home(i):
        return link(combined.at[z], zrx.at[above(i)], b_send.at[above(i)], b_recv.at[above(i)], (s, 2 * above(i) + c))

    for i in range(1, nz):
        home(i).wait_recv()

    def finish(r):
        total = mine[r, :]
        for i in range(1, nz):
            total = total + zrx[above(i), r, :].astype(jnp.float32)
        out[r, :] = (hidden[z, r, :].astype(jnp.float32) + total).astype(jnp.bfloat16)

    by_rows(0, rows, finish)
    left = halo + given + [lent] + [note(i) for i in range(1, nz)]
    if relayed:
        left += [side_note] + [raw_copy(b) for b in range(nz)] + [side_copy(b) for b in range(nz)]
    left += [swap(b) for b in range(nz)] + sum([return_copies(b) for b in range(nz)], [])
    left += [homeward(above(i)) for i in range(1, nz)]
    for copy in left:
        copy.wait_send()

    @pl.when(z < nz - 1)
    def sent_up():
        for q in range(pieces):
            upward(q).wait_send()

    @pl.when(z > 0)
    def sent_down():
        for q in range(pieces):
            downward(q).wait_send()


def shards(
    out_gate,
    in_gate,
    conv_input,
    conv_taps,
    documents,
    out_weight,
    residual,
    norm_gain,
    expert_ids,
    route_weights,
    gate_weight,
    up_weight,
    down_weight,
):
    n_sp, nz = lax.axis_size("sp"), lax.axis_size("tp") // 2
    length, channels = conv_input.shape
    rows, width = residual.shape
    units = gate_weight.shape[2]
    capacity = max(2, (3 * rows + n_sp - 1) // n_sp)
    cap = -(-capacity // CHUNK) * CHUNK
    relayed = n_sp == 4
    pieces = nz * (rows // min(PIECE, rows))
    bf16, f32, dma = jnp.bfloat16, jnp.float32, pltpu.SemaphoreType.DMA
    hbm = pl.BlockSpec(memory_space=pltpu.HBM)
    per_z = pltpu.VMEM((nz, rows, width), bf16)
    per_z_side = per_z if relayed else pltpu.VMEM((1, CHUNK, LANES), bf16)
    slots = pltpu.VMEM((nz, n_sp, cap, width), bf16)
    return pl.pallas_call(
        functools.partial(layer_kernel, n_sp, nz, cap),
        out_shape=jax.ShapeDtypeStruct((rows, width), bf16),
        in_specs=[hbm] * 13,
        out_specs=pl.BlockSpec(memory_space=pltpu.VMEM),
        scratch_shapes=[
            pltpu.VMEM((length, channels), bf16),
            pltpu.VMEM((length, channels), bf16),
            pltpu.VMEM((length, channels), bf16),
            pltpu.VMEM(conv_taps.shape, bf16),
            pltpu.VMEM((length,), jnp.int32),
            pltpu.VMEM((rows, width), bf16),
            pltpu.VMEM((width,), bf16),
            pltpu.VMEM((2, rows), jnp.int32),
            pltpu.VMEM((2, rows), f32),
            pltpu.VMEM((width, units), bf16),
            pltpu.VMEM((width, units), bf16),
            pltpu.VMEM((units, width), bf16),
            pltpu.VMEM((HALO + length, channels), f32),
            pltpu.VMEM((HALO + length, LANES), f32),
            pltpu.VMEM((HALO, channels), f32),
            pltpu.VMEM((HALO, LANES), f32),
            pltpu.VMEM((HALO, channels), f32),
            pltpu.VMEM((HALO, LANES), f32),
            pltpu.VMEM((2 * nz, rows, channels), bf16),
            pltpu.VMEM((nz, rows, channels), bf16),
            pltpu.VMEM((2, channels, width), bf16),
            pltpu.VMEM((nz, rows, width), f32),
            per_z,
            per_z,
            per_z,
            per_z,
            per_z,
            per_z,
            pltpu.VMEM((8, rows), f32),
            pltpu.VMEM((nz, 8, rows), f32),
            pltpu.VMEM((nz, 8, rows), f32),
            per_z_side,
            slots,
            pltpu.VMEM((nz, 2, n_sp, cap, width), bf16),
            pltpu.VMEM((2 * n_sp * cap, units), bf16),
            slots,
            pltpu.VMEM((nz, 2 if relayed else n_sp, cap, width), bf16),
            per_z_side,
            per_z_side,
            pltpu.VMEM((rows, width), f32),
            per_z,
            per_z,
            dma((13,)),
            dma((2,)),
            dma((2,)),
            dma((nz,)),
            dma((nz,)),
            dma((1,)),
            dma((1,)),
            dma((1,)),
            dma((1,)),
            dma((nz,)),
            dma((nz,)),
            dma((pieces,)),
            dma((pieces,)),
            dma((pieces,)),
            dma((pieces,)),
            dma((nz,)),
            dma((nz,)),
            dma((nz, n_sp)),
            dma((nz, n_sp)),
            dma((nz,)),
            dma((nz,)),
            dma((nz,)),
            dma((nz,)),
            dma((nz, n_sp)),
            dma((nz, n_sp)),
            dma((nz,)),
            dma((nz,)),
            dma((nz,)),
            dma((nz,)),
        ],
        compiler_params=pltpu.CompilerParams(
            collective_id=0, has_side_effects=True, vmem_limit_bytes=VMEM_LIMIT
        ),
    )(
        in_gate, conv_input, out_gate, conv_taps, documents, out_weight, residual, norm_gain, expert_ids.T,
        route_weights.T, gate_weight[0], up_weight[0], down_weight[0],
    )


def solution(mesh):
    in_specs = (
        P("sp", "tp"),
        P("sp", "tp"),
        P("sp", "tp"),
        P(None, "tp"),
        P("sp"),
        P("tp", None),
        P(("sp", "tp"), None),
        P(),
        P(("sp", "tp"), None),
        P(("sp", "tp"), None),
        P("sp", None, "tp"),
        P("sp", None, "tp"),
        P("sp", "tp", None),
    )
    out_specs = P(("sp", "tp"), None)
    return jax.shard_map(shards, mesh=mesh, in_specs=in_specs, out_specs=out_specs, check_vma=False)
```

```python
import functools

import jax
import jax.numpy as jnp
from jax import lax
from jax.experimental import pallas as pl
from jax.experimental.pallas import tpu as pltpu
from jax.sharding import PartitionSpec as P

EPS = 1e-06


MESH = pl.DeviceIdType.MESH
CHUNK = 16
COLS = 512
UNITS = 256
HALO = 8
PIECE = 16
LAG = 3
LANES = 128
VMEM_LIMIT = 63 * 1024 * 1024


def turn(nz, a):
    return (nz - 1 - a // 2) if a % 2 == 0 else a // 2


def where_am_i():
    s, t = lax.axis_index("sp"), lax.axis_index("tp")
    return s, t // 2, t % 2


def greet(s, z, c, n_sp, nz):
    barrier = pltpu.get_barrier_semaphore()
    peers = [(s, 2 * z + 1 - c)]
    peers += [(s, 2 * lax.rem(z + i, nz) + c) for i in range(1, nz)]
    peers += [(lax.rem(s + k, n_sp), 2 * z + c) for k in range(1, n_sp)]
    for peer in peers:
        pl.semaphore_signal(barrier, inc=1, device_id=peer, device_id_type=MESH)
    return lambda: pl.semaphore_wait(barrier, len(peers))


def link(src, dst, send_sem, recv_sem, peer):
    return pltpu.make_async_remote_copy(
        src_ref=src,
        dst_ref=dst,
        send_sem=send_sem,
        recv_sem=recv_sem,
        device_id=peer,
        device_id_type=MESH,
    )


def by_rows(first, count, body):
    def step(r, carry):
        body(pl.ds(pl.multiple_of(first + r * CHUNK, CHUNK), CHUNK))
        return carry

    lax.fori_loop(0, count // CHUNK, step, 0)


def by_columns(width, body):
    def step(r, carry):
        body(pl.ds(pl.multiple_of(r * COLS, COLS), COLS))
        return carry

    lax.fori_loop(0, width // COLS, step, 0)


def slot_hits(meta, experts, cap):
    rows = meta.shape[1]
    slots = lax.broadcasted_iota(jnp.int32, (len(experts) * cap, rows), 0).astype(jnp.float32)
    hits = []
    for k in range(2):
        at = jnp.full((1, rows), -1.0, jnp.float32)
        for a, expert in enumerate(experts):
            at = jnp.where(meta[2 * k : 2 * k + 1, :] == expert, float(a * cap) + meta[2 * k + 1 : 2 * k + 2, :], at)
        hits.append(slots == at)
    return hits


def slot_table(meta, experts, cap):
    first, second = slot_hits(meta, experts, cap)
    return (first | second).astype(jnp.float32).astype(jnp.bfloat16)


def slot_weights(meta, experts, cap):
    first, second = slot_hits(meta, experts, cap)
    weights = jnp.where(first, meta[4:5, :], 0.0) + jnp.where(second, meta[5:6, :], 0.0)
    high = weights.astype(jnp.bfloat16)
    return high, (weights - high.astype(jnp.float32)).astype(jnp.bfloat16)


def weigh(weights, values):
    dims = (((0,), (0,)), ((), ()))
    total = lax.dot_general(weights[0], values, dims, preferred_element_type=jnp.float32)
    return total + lax.dot_general(weights[1], values, dims, preferred_element_type=jnp.float32)


def describe(ids, shares, meta, n_sp):
    rows = ids.shape[1]
    named_ids = ids[...].astype(jnp.float32)
    choice = [named_ids[0:1, :], named_ids[1:2, :]]
    expert = lax.broadcasted_iota(jnp.int32, (-(-n_sp // CHUNK) * CHUNK, rows), 0).astype(jnp.float32)
    names = [expert == choice[0], expert == choice[1]]
    named = (names[0] | names[1]).astype(jnp.float32).astype(jnp.bfloat16)
    before = lax.broadcasted_iota(jnp.int32, (rows, rows), 0) < lax.broadcasted_iota(jnp.int32, (rows, rows), 1)
    earlier = jnp.dot(
        named, before.astype(jnp.float32).astype(jnp.bfloat16), preferred_element_type=jnp.float32
    )
    for k in range(2):
        meta[2 * k : 2 * k + 1, :] = choice[k]
        meta[2 * k + 1 : 2 * k + 2, :] = jnp.sum(jnp.where(names[k], earlier, 0.0), axis=0, keepdims=True)
    meta[4:6, :] = shares[...]
    meta[6:8, :] = jnp.zeros((2, rows), jnp.float32)


def layer_kernel(
    n_sp, nz, cap,
    in_gate_hbm, conv_input_hbm, out_gate_hbm, taps_hbm, docs_hbm, out_weight_hbm, residual_hbm, gain_hbm, ids_hbm,
    shares_hbm, gate_hbm, up_hbm, down_hbm,
    out,
    in_gate, conv_input, out_gate, taps, docs, residual, gain, ids, shares, gate, up, down,
    signal, long_docs, tail_signal, tail_docs, halo_signal, halo_docs,
    gated, other_gated, weight, part, from_low, from_high, to_high, to_low, hidden, nbuf,
    meta, metas, side_metas, raw, routed, gathered, act, half_rx, arrived, side_sum, side_rx, mine, combined, zrx,
    w_sem, h_send, h_recv, m_send, m_recv, x_send, x_recv, v_send, v_recv, o_send, o_recv,
    u_send, u_recv, d_send, d_recv, g_send, g_recv, p_send, p_recv, f_send, f_recv,
    e_send, e_recv, r_send, r_recv, k_send, k_recv, b_send, b_recv,
):
    s, z, c = where_am_i()
    o = 1 - c
    relayed = n_sp == 4
    partner = (s, 2 * z + o)
    rows, width = residual.shape
    length, channels = in_gate.shape
    piece = min(PIECE, rows)
    per = rows // piece
    pieces = nz * per
    order = [turn(nz, a) for a in range(nz)]
    greeted = greet(s, z, c, n_sp, nz)
    loads = [
        pltpu.make_async_copy(src, dst, w_sem.at[i])
        for i, (src, dst) in enumerate(
            [
                (in_gate_hbm, in_gate), (conv_input_hbm, conv_input), (docs_hbm, docs), (taps_hbm, taps),
                (ids_hbm, ids), (shares_hbm, shares), (out_gate_hbm, out_gate), (out_weight_hbm, weight.at[0]),
                (residual_hbm, residual), (gain_hbm, gain), (gate_hbm, gate), (up_hbm, up), (down_hbm, down),
            ]
        )
    ]
    for load in loads:
        load.start()

    @pl.when(z == 0)
    def no_lower():
        from_low[...] = jnp.zeros_like(from_low)

    @pl.when(z == nz - 1)
    def no_higher():
        from_high[...] = jnp.zeros_like(from_high)

    def above(i):
        return lax.rem(z + i, nz)

    def on_plane(k):
        return lax.rem(s + k, n_sp)

    if relayed:
        right, down_one = 1 - 2 * (s % 2), 2 - 4 * (s // 2)
        side = s + (1 - c) * right + c * down_one
        cross = s + c * right + (1 - c) * down_one
        side_peer, cross_peer = (side, 2 * z + c), (cross, 2 * z + c)
        experts = [s.astype(jnp.float32), cross.astype(jnp.float32)]
    else:
        experts = [on_plane(k).astype(jnp.float32) for k in range(n_sp)]

    for load in loads[:6]:
        load.wait()
    signal[HALO:, :] = in_gate[...].astype(jnp.float32) * conv_input[...].astype(jnp.float32)
    row = jnp.broadcast_to(docs[...].astype(jnp.float32).reshape(1, length), (CHUNK, length))
    one = (lax.broadcasted_iota(jnp.int32, (CHUNK, LANES), 0) == 0).astype(jnp.float32).astype(jnp.bfloat16)
    long_docs[HALO:, :] = lax.dot_general(
        row.astype(jnp.bfloat16), one, (((0,), (0,)), ((), ())), preferred_element_type=jnp.float32
    )
    tail_signal[...] = signal[length : length + HALO, :]
    tail_docs[...] = long_docs[length : length + HALO, :]
    describe(ids, shares, meta, n_sp)
    metas[z] = meta[...]
    loads[6].wait()
    tap_values = taps[...].astype(jnp.float32)

    def convolve(strip):
        r = strip * rows
        at = [slice(HALO + r - j, HALO + r - j + rows) for j in range(3)]
        here = long_docs[at[0], :]
        same = [None] + [long_docs[at[j], :] == here for j in (1, 2)]
        for l in range(0, channels, LANES):
            lane = slice(l, l + LANES)
            conv = tap_values[2:3, lane] * signal[at[0], lane]
            for j in (1, 2):
                conv = conv + jnp.where(same[j], tap_values[2 - j : 3 - j, lane] * signal[at[j], lane], 0.0)
            gated[strip, :, lane] = (out_gate[r : r + rows, lane].astype(jnp.float32) * conv).astype(jnp.bfloat16)

    for strip in range(2 * nz - 1, 0, -1):
        convolve(strip)
    loads[7].wait()
    greeted()
    following = (on_plane(1), 2 * z + c)
    halo = [
        link(tail_signal, halo_signal, h_send.at[0], h_recv.at[0], following),
        link(tail_docs, halo_docs, h_send.at[1], h_recv.at[1], following),
    ]
    given = [
        link(gated.at[2 * b + o], other_gated.at[b], o_send.at[b], o_recv.at[b], partner) for b in range(nz)
    ]
    lent = [
        link(
            weight.at[0, :, pl.ds(l, COLS)], weight.at[1, :, pl.ds(l, COLS)], v_send.at[i], v_recv.at[i], partner
        )
        for i, l in enumerate(range(0, width, COLS))
    ]
    for copy in halo:
        copy.start()
    given[nz - 1].start()
    for copy in lent:
        copy.start()
    for b in order[2:]:
        given[b].start()

    def note(i):
        return link(meta, metas.at[z], m_send.at[i], m_recv.at[z], (s, 2 * above(i) + c))

    def noted(i):
        return link(meta, metas.at[above(i)], m_send.at[i], m_recv.at[above(i)], (s, 2 * above(i) + c))

    for i in range(1, nz):
        note(i).start()
    side_note = link(metas, side_metas, x_send.at[0], x_recv.at[0], side_peer) if relayed else None

    def place(q):
        return order[q // per], (q % per) * piece

    def upward(q):
        b, first = place(q)
        at = pl.ds(first, piece)
        return link(to_high.at[b, at], from_low.at[b, at], u_send.at[q], u_recv.at[q], (s, 2 * above(1) + c))

    def downward(q):
        b, first = place(q)
        at = pl.ds(first, piece)
        return link(to_low.at[b, at], from_high.at[b, at], d_send.at[q], d_recv.at[q], (s, 2 * above(nz - 1) + c))

    def pass_on(q, came, going, copy):
        b, first = place(q)

        def add(r):
            going[b, r, :] = (part[b, r, :] + came[b, r, :].astype(jnp.float32)).astype(jnp.bfloat16)

        by_rows(first, piece, add)
        copy(q).start()

    def project(b):
        given[b].wait_recv()

        def columns(cols):
            part[b, :, cols] = jnp.dot(
                gated[2 * b + c], weight[0, :, cols], preferred_element_type=jnp.float32
            ) + jnp.dot(other_gated[b], weight[1, :, cols], preferred_element_type=jnp.float32)

        if b == order[0]:
            for i, copy in enumerate(lent):
                copy.wait_recv()
                columns(pl.ds(i * COLS, COLS))
        else:
            by_columns(width, columns)

        @pl.when(z == b)
        def own():
            def add(r):
                part[b, r, :] = part[b, r, :] + residual[r, :].astype(jnp.float32)

            by_rows(0, rows, add)

    loads[8].wait()
    for a, b in enumerate(order):
        if b == 0:
            for copy in halo:
                copy.wait_recv()
            signal[:HALO, :] = halo_signal[...]
            long_docs[:HALO, :] = jnp.where(s == 0, -1.0, halo_docs[...])
            convolve(0)
            given[0].start()
        project(b)
        for q in range(a * per, (a + 1) * per):

            @pl.when(z == 0)
            def lowest(q=q):
                pass_on(q, from_low, to_high, upward)

            @pl.when(z == nz - 1)
            def highest(q=q):
                pass_on(q, from_high, to_low, downward)

    for i in range(1, nz):
        noted(i).wait_recv()
    if relayed:
        side_note.start()
    loads[9].wait()

    def from_below(q):
        @pl.when(z > 0)
        def some():
            upward(q).wait_recv()

        @pl.when((z > 0) & (z < nz - 1))
        def middle():
            pass_on(q, from_low, to_high, upward)

    def from_above(q):
        @pl.when(z < nz - 1)
        def some():
            downward(q).wait_recv()

        @pl.when((z > 0) & (z < nz - 1))
        def middle():
            pass_on(q, from_high, to_low, downward)

    def norm(q):
        b, first = place(q)

        def rows_of(r):
            total = part[b, r, :] + from_low[b, r, :].astype(jnp.float32) + from_high[b, r, :].astype(jnp.float32)
            state = total.astype(jnp.bfloat16)
            hidden[b, r, :] = state
            wide = state.astype(jnp.float32)
            stats = jnp.mean(wide * wide, axis=-1, keepdims=True)
            scale = gain[...].astype(jnp.float32).reshape(1, width)
            nbuf[b, r, :] = (wide * lax.rsqrt(stats + EPS) * scale).astype(jnp.bfloat16)

        by_rows(first, piece, rows_of)

    def raw_copy(b, h):
        at = pl.ds(h * (rows // 2), rows // 2)
        return link(nbuf.at[b, at], raw.at[b, at], g_send.at[b, h], g_recv.at[b, h], side_peer)

    def send_half(b):
        if relayed:
            raw_copy(b, 0).start()

    def slot_copies(b, those=(0, 1)):
        if relayed:
            return [
                link(routed.at[b, k], gathered.at[b, 0, 2 + k], p_send.at[b, k], p_recv.at[b, k], cross_peer)
                for k in those
            ]
        return [
            link(
                routed.at[b, k], gathered.at[b, 0, k], p_send.at[b, k], p_recv.at[b, k], (on_plane(k), 2 * z + c)
            )
            for k in range(1, n_sp)
        ]

    def send_rest(b):
        if relayed:
            raw_copy(b, 1).start()

    def dispatch(b):
        table = slot_table(metas[b], experts, cap)

        def columns(cols):
            placed = jnp.dot(table, nbuf[b, :, cols], preferred_element_type=jnp.float32).astype(jnp.bfloat16)
            gathered[b, 0, 0, :, cols] = placed[:cap]
            for k in range(1, len(experts)):
                routed[b, k - 1 if relayed else k, :, cols] = placed[k * cap : (k + 1) * cap]

        by_columns(width, columns)
        for copy in slot_copies(b, (0,)):
            copy.start()

    def relay(b):
        if not relayed:
            return
        for h in range(2):
            raw_copy(b, h).wait_recv()
        table = slot_table(side_metas[b], experts, cap)

        def columns(cols):
            placed = jnp.dot(table, raw[b, :, cols], preferred_element_type=jnp.float32).astype(jnp.bfloat16)
            gathered[b, 0, 1, :, cols] = placed[:cap]
            routed[b, 1, :, cols] = placed[cap:]

        by_columns(width, columns)
        slot_copies(b, (1,))[0].start()
        forwards(b)[0].start()

    def forwards(b):
        parts = 2 if relayed else 1
        count = n_sp // parts
        return [
            link(
                gathered.at[b, 0, pl.ds(h * count, count)], gathered.at[b, 1, pl.ds(h * count, count)],
                f_send.at[b, h], f_recv.at[b, h], partner,
            )
            for h in range(parts)
        ]

    def unless_own(b, act_on):
        @pl.when(z != b)
        def other():
            act_on(b)

    for t in range(pieces + LAG):

        @pl.when(z < nz // 2)
        def lower(t=t):
            if t < pieces:
                from_below(t)
            if t >= LAG:
                from_above(t - LAG)

        @pl.when(z >= nz // 2)
        def upper(t=t):
            if t < pieces:
                from_above(t)
            if t >= LAG:
                from_below(t - LAG)

        q = t - LAG
        if q >= 0:
            if q == 0 and relayed:
                side_note.wait_recv()
            norm(q)
            a = q // per
            if q % per == max(per // 2 - 1, 0) and a >= 2:
                unless_own(order[a - 2], relay)
            if q % per == per // 2 - 1:
                unless_own(order[a], send_half)
            if q % per == per - 1:
                unless_own(order[a], send_rest)
                unless_own(order[a], dispatch)
    own_turn = jnp.where(z >= nz // 2, 2 * (nz - 1 - z), 2 * z + 1)

    def at_step(j):
        if j == nz - 1:
            return z
        if j >= nz - 3:
            j = jnp.where(z == nz - 1, 2 * nz - 5 - j, j)
        a = j + jnp.where(j >= own_turn, 1, 0)
        return jnp.where(a % 2 == 0, nz - 1 - a // 2, a // 2)

    def swap(b, r):
        cols = pl.ds(pl.multiple_of(r * COLS, COLS), COLS)
        return link(
            gathered.at[b, 0, :, :, cols], half_rx.at[b, :, :, cols], e_send.at[b, r], e_recv.at[b, r], partner
        )

    def return_copies(b):
        if relayed:
            return [
                link(routed.at[b, 2 + k], arrived.at[b, k], r_send.at[b, k], r_recv.at[b, k], cross_peer)
                for k in range(2)
            ]
        return [
            link(
                routed.at[b, k], arrived.at[b, k], r_send.at[b, k], r_recv.at[b, k], (on_plane(n_sp - k), 2 * z + c)
            )
            for k in range(1, n_sp)
        ]

    def side_copy(b):
        return link(side_sum.at[b], side_rx.at[b], k_send.at[b], k_recv.at[b], side_peer)

    def gather(j):
        b = at_step(j)
        for copy in slot_copies(b):
            copy.wait_recv()
        forwards(b)[-1].start()

    def expert(j):
        b = at_step(j)
        if j == 0:
            for load in loads[10:]:
                load.wait()
        for copy in forwards(b):
            copy.wait_recv()
        half = n_sp * cap
        hidden_units = gate.shape[1]
        step = min(UNITS, hidden_units)

        def inner(r, carry):
            units = pl.ds(pl.multiple_of(r * step, step), step)
            held = gathered[b].reshape(2 * half, width)
            gate_proj = jnp.dot(held, gate[:, units], preferred_element_type=jnp.float32)
            up_proj = jnp.dot(held, up[:, units], preferred_element_type=jnp.float32)
            act[:, units] = (gate_proj / (1.0 + jnp.exp(-gate_proj)) * up_proj).astype(jnp.bfloat16)
            return carry

        lax.fori_loop(0, hidden_units // step, inner, 0)
        for copy in slot_copies(b):
            copy.wait_send()
        for copy in forwards(b):
            copy.wait_send()

        def outer(r, carry):
            cols = pl.ds(pl.multiple_of(r * COLS, COLS), COLS)
            share = jnp.dot(act[...], down[:, cols], preferred_element_type=jnp.float32).astype(jnp.bfloat16)
            routed[b, :, :, cols] = share[:half].reshape(n_sp, cap, COLS)
            gathered[b, 0, :, :, cols] = share[half:].reshape(n_sp, cap, COLS)
            swap(b, r).start()
            return carry

        lax.fori_loop(0, width // COLS, outer, 0)

    def give_back(j):
        b = at_step(j)

        def add(first, count, waiting=False):
            def columns(r, carry):
                if waiting:
                    swap(b, r).wait_recv()
                cols, at = pl.ds(pl.multiple_of(r * COLS, COLS), COLS), pl.ds(first, count)
                total = routed[b, at, :, cols].astype(jnp.float32) + half_rx[b, at, :, cols].astype(jnp.float32)
                routed[b, at, :, cols] = total.astype(jnp.bfloat16)
                return carry

            lax.fori_loop(0, width // COLS, columns, 0)

        if relayed:
            add(3, 1, True)
            return_copies(b)[1].start()
            add(2, 1)
            return_copies(b)[0].start()
            add(0, 2)
        else:
            add(0, n_sp, True)
            for copy in return_copies(b):
                copy.start()

    def relay_back(j):
        if not relayed:
            return
        b = at_step(j)
        return_copies(b)[1].wait_recv()
        weights = slot_weights(side_metas[b], experts, cap)

        def columns(cols):
            values = jnp.concatenate([routed[b, 1, :, cols], arrived[b, 1, :, cols]], axis=0)
            side_sum[b, :, cols] = weigh(weights, values).astype(jnp.bfloat16)

        by_columns(width, columns)
        side_copy(b).start()

    def homeward(b):
        return link(combined.at[b], zrx.at[z], b_send.at[b], b_recv.at[z], (s, 2 * b + c))

    def collect(j):
        b = at_step(j)
        for copy in [return_copies(b)[0], side_copy(b)] if relayed else return_copies(b):
            copy.wait_recv()
        weights = slot_weights(metas[b], experts, cap)

        def columns(cols):
            parts = [routed[b, 0, :, cols]]
            if relayed:
                parts.append(arrived[b, 0, :, cols])
            else:
                parts += [arrived[b, k, :, cols] for k in range(1, n_sp)]
            total = weigh(weights, jnp.concatenate(parts, axis=0))
            if relayed:
                total = total + side_rx[b, :, cols].astype(jnp.float32)
            if j < nz - 1:
                combined[b, :, cols] = total.astype(jnp.bfloat16)
            else:
                mine[:, cols] = total

        by_columns(width, columns)
        if j < nz - 1:
            homeward(b).start()

    send_half(z)
    send_rest(z)
    unless_own(order[-2], relay)
    dispatch(z)
    gather(0)
    expert(0)
    unless_own(order[-1], relay)
    for j in range(1, nz):
        give_back(j - 1)
        gather(j)
        expert(j)
        if j == 1:
            relay(z)
        relay_back(j - 1)
        if j == nz - 1:
            give_back(j)
        if j >= 2:
            collect(j - 2)
    relay_back(nz - 1)
    collect(nz - 2)
    collect(nz - 1)

    def home(i):
        return link(combined.at[z], zrx.at[above(i)], b_send.at[above(i)], b_recv.at[above(i)], (s, 2 * above(i) + c))

    for i in range(1, nz):
        home(i).wait_recv()

    def finish(r):
        total = mine[r, :]
        for i in range(1, nz):
            total = total + zrx[above(i), r, :].astype(jnp.float32)
        out[r, :] = (hidden[z, r, :].astype(jnp.float32) + total).astype(jnp.bfloat16)

    by_rows(0, rows, finish)
    left = halo + given + lent + [note(i) for i in range(1, nz)]
    if relayed:
        left += [side_note] + [raw_copy(b, h) for b in range(nz) for h in range(2)] + [side_copy(b) for b in range(nz)]
    left += [swap(b, r) for b in range(nz) for r in range(width // COLS)] + sum([return_copies(b) for b in range(nz)], [])
    left += [homeward(above(i)) for i in range(1, nz)]
    for copy in left:
        copy.wait_send()

    @pl.when(z < nz - 1)
    def sent_up():
        for q in range(pieces):
            upward(q).wait_send()

    @pl.when(z > 0)
    def sent_down():
        for q in range(pieces):
            downward(q).wait_send()


def shards(
    out_gate,
    in_gate,
    conv_input,
    conv_taps,
    documents,
    out_weight,
    residual,
    norm_gain,
    expert_ids,
    route_weights,
    gate_weight,
    up_weight,
    down_weight,
):
    n_sp, nz = lax.axis_size("sp"), lax.axis_size("tp") // 2
    length, channels = conv_input.shape
    rows, width = residual.shape
    units = gate_weight.shape[2]
    capacity = max(2, (3 * rows + n_sp - 1) // n_sp)
    cap = -(-capacity // CHUNK) * CHUNK
    relayed = n_sp == 4
    pieces = nz * (rows // min(PIECE, rows))
    bf16, f32, dma = jnp.bfloat16, jnp.float32, pltpu.SemaphoreType.DMA
    hbm = pl.BlockSpec(memory_space=pltpu.HBM)
    per_z = pltpu.VMEM((nz, rows, width), bf16)
    per_z_side = per_z if relayed else pltpu.VMEM((1, CHUNK, LANES), bf16)
    slots = pltpu.VMEM((nz, n_sp, cap, width), bf16)
    return pl.pallas_call(
        functools.partial(layer_kernel, n_sp, nz, cap),
        out_shape=jax.ShapeDtypeStruct((rows, width), bf16),
        in_specs=[hbm] * 13,
        out_specs=pl.BlockSpec(memory_space=pltpu.VMEM),
        scratch_shapes=[
            pltpu.VMEM((length, channels), bf16),
            pltpu.VMEM((length, channels), bf16),
            pltpu.VMEM((length, channels), bf16),
            pltpu.VMEM(conv_taps.shape, bf16),
            pltpu.VMEM((length,), jnp.int32),
            pltpu.VMEM((rows, width), bf16),
            pltpu.VMEM((width,), bf16),
            pltpu.VMEM((2, rows), jnp.int32),
            pltpu.VMEM((2, rows), f32),
            pltpu.VMEM((width, units), bf16),
            pltpu.VMEM((width, units), bf16),
            pltpu.VMEM((units, width), bf16),
            pltpu.VMEM((HALO + length, channels), f32),
            pltpu.VMEM((HALO + length, LANES), f32),
            pltpu.VMEM((HALO, channels), f32),
            pltpu.VMEM((HALO, LANES), f32),
            pltpu.VMEM((HALO, channels), f32),
            pltpu.VMEM((HALO, LANES), f32),
            pltpu.VMEM((2 * nz, rows, channels), bf16),
            pltpu.VMEM((nz, rows, channels), bf16),
            pltpu.VMEM((2, channels, width), bf16),
            pltpu.VMEM((nz, rows, width), f32),
            per_z,
            per_z,
            per_z,
            per_z,
            per_z,
            per_z,
            pltpu.VMEM((8, rows), f32),
            pltpu.VMEM((nz, 8, rows), f32),
            pltpu.VMEM((nz, 8, rows), f32),
            per_z_side,
            slots,
            pltpu.VMEM((nz, 2, n_sp, cap, width), bf16),
            pltpu.VMEM((2 * n_sp * cap, units), bf16),
            slots,
            pltpu.VMEM((nz, 2 if relayed else n_sp, cap, width), bf16),
            per_z_side,
            per_z_side,
            pltpu.VMEM((rows, width), f32),
            per_z,
            per_z,
            dma((13,)),
            dma((2,)),
            dma((2,)),
            dma((nz,)),
            dma((nz,)),
            dma((1,)),
            dma((1,)),
            dma((width // COLS,)),
            dma((width // COLS,)),
            dma((nz,)),
            dma((nz,)),
            dma((pieces,)),
            dma((pieces,)),
            dma((pieces,)),
            dma((pieces,)),
            dma((nz, 2)),
            dma((nz, 2)),
            dma((nz, n_sp)),
            dma((nz, n_sp)),
            dma((nz, 2)),
            dma((nz, 2)),
            dma((nz, width // COLS)),
            dma((nz, width // COLS)),
            dma((nz, n_sp)),
            dma((nz, n_sp)),
            dma((nz,)),
            dma((nz,)),
            dma((nz,)),
            dma((nz,)),
        ],
        compiler_params=pltpu.CompilerParams(
            collective_id=0, has_side_effects=True, vmem_limit_bytes=VMEM_LIMIT
        ),
    )(
        in_gate, conv_input, out_gate, conv_taps, documents, out_weight, residual, norm_gain, expert_ids.T,
        route_weights.T, gate_weight[0], up_weight[0], down_weight[0],
    )


def solution(mesh):
    in_specs = (
        P("sp", "tp"),
        P("sp", "tp"),
        P("sp", "tp"),
        P(None, "tp"),
        P("sp"),
        P("tp", None),
        P(("sp", "tp"), None),
        P(),
        P(("sp", "tp"), None),
        P(("sp", "tp"), None),
        P("sp", None, "tp"),
        P("sp", None, "tp"),
        P("sp", "tp", None),
    )
    out_specs = P(("sp", "tp"), None)
    return jax.shard_map(shards, mesh=mesh, in_specs=in_specs, out_specs=out_specs, check_vma=False)
```
